256 devices in a mesh: grp: 4 (over y, x), ep: 32 (over z), tp: 2 (over core).
Axes of the slice: x: 2, y: 2, z: 32, core: 2. Of those that a mesh axis runs over, the one named last changes fastest.
The devices are a block of a 4x16x32 slice.
Arguments:
- tokens: bfloat16 [8192, 2048], P(('grp', 'ep')), parts along dimension 0, may hold values from -6 to 6
- norm_gain: float32 [2048], replicated, may hold values from 0.1 to 1.9
- expert_gate: bfloat16 [32, 2048, 512], P('ep', None, 'tp'), may hold values from -0.125 to 0.125
- expert_up: bfloat16 [32, 2048, 512], P('ep', None, 'tp'), may hold values from -0.125 to 0.125
- expert_down: bfloat16 [32, 512, 2048], P('ep', 'tp'), may hold values from -0.25 to 0.25
- shared_gate: bfloat16 [2048, 512], P(None, 'tp'), may hold values from -0.125 to 0.125
- shared_up: bfloat16 [2048, 512], P(None, 'tp'), may hold values from -0.125 to 0.125
- shared_down: bfloat16 [512, 2048], P('tp'), may hold values from -0.25 to 0.25
- routes: int32 [8192, 8], P(('grp', 'ep')), parts along dimension 0, may hold values from 0 to 31, all different within a row; in each aligned block of 64 rows (0 to 63, 64 to 127, ...) at most 32 rows name the same one
- route_weights: float32 [8192, 8], P(('grp', 'ep')), parts along dimension 0, may hold values from 0.05 to 0.6
Outputs:
- mixed: bfloat16 [8192, 2048], P(('grp', 'ep'), 'tp'), parts along dimension 0
The draws below stay inside these ranges and needn't reach their ends.
There are 4 independent parts, one for each index of `grp`. The reference program is written for one: setup_inputs(seed, part) draws one part's arguments, and reference() takes and returns one part's arrays. A program takes and returns all parts, laid end to end along the dimension named above; an argument that names none is the same for every part. Nothing has to cross between parts.
Inputs may be any that keep to these rules, and one draw needn't show every extreme that they name: `routes`: each row names 8 different experts. Within the rows of one index of ep no expert is named more than 32 times, a bound that some block reaches by the rows of some index of ep.
All inputs are finite; a program needn't handle non-finite values.
Results may differ from the reference program's by a relative error of at most 0.0085.
Values may be sent and summed in bfloat16 or wider, within the bound.
No kernel may reach another device: no remote copies, remote signals or barrier semaphores. Data moves between devices by JAX's collectives and lax.ppermute only.
A program may use at most 64 MiB of HBM per device.

```python
import math
import jax
import jax.numpy as jnp
import numpy as np
from jax import lax

D = 2048
FF_E = 512
FF_S = 512
TOP_K = 8
TOK_DEV = 64
EXPERTS = 32
TOKENS = 2048
CAP = 32
N_TP = 2


def block_scale(key, dims, cuts, least, top_value):
    loudness, own = 1.0, jax.random.fold_in(key, 6)
    for position, blocks in cuts:
        draws = jnp.exp(jax.random.uniform(jax.random.fold_in(own, position), (blocks,), jnp.float32, least / len(cuts), top_value / len(cuts)))
        loudness = loudness * jnp.repeat(draws, dims[position] // blocks).reshape([-1 if axis == position else 1 for axis in range(len(dims))])
    return loudness


def routed_block(stream_key, own, number, rows, count, top, limit, slope):
    order = jax.random.permutation(stream_key, count)
    heavy_load, usual = shares(count, rows * top, limit, slope, True), shares(count, rows * top, limit, slope, False)
    places = jnp.arange(count)

    def named(tallies, offset_by):
        used = int((tallies > 0).sum())
        fixed = max(1, used // 4)
        shifted = fixed + (places - fixed + offset_by * (used - fixed)) % max(1, count - fixed)
        return jnp.zeros((count,), jnp.int32).at[order[jnp.where(places < fixed, places, shifted)]].set(jnp.asarray(tallies, jnp.int32))

    tallies = jnp.where(number % 4 == 0, named(heavy_load, number // 4), named(usual, number - number // 4 - 1))
    mixed = jax.random.permutation(jax.random.fold_in(own, 3), count)
    donor, sink = mixed[0:count // 2 * 2:2], mixed[1:count // 2 * 2:2]
    room = jnp.minimum(tallies[donor] - 1, limit - tallies[sink]) // 2
    room = jnp.where((donor == order[0]) | (sink == order[0]) | (tallies[sink] == 0), 0, jnp.maximum(room, 0))
    shifted = jax.random.randint(jax.random.fold_in(own, 4), (count // 2,), 0, 1 << 20) % (room + 1)
    tallies = tallies.at[donor].add(-shifted).at[sink].add(shifted)
    labels = jnp.searchsorted(jnp.cumsum(tallies), jnp.arange(rows * top), side="right").astype(jnp.int32)
    listing = labels.reshape(top, rows).T
    listing = listing[jax.random.permutation(jax.random.fold_in(own, 1), rows)]
    offset_by = jax.random.randint(jax.random.fold_in(own, 2), (rows, 1), 0, top)
    return jnp.take_along_axis(listing, (jnp.arange(top)[None, :] + offset_by) % top, axis=1)


def shares(number_of, total, reach, skew, full):
    loads = [(1 << 20) // math.isqrt(standing ** skew) + 1 for standing in range(1, number_of + 1)]
    largest = reach if full else min(reach, max(-(-total // number_of), total * loads[0] // sum(loads)))
    least = 1 if total - largest >= number_of - 1 else 0
    counts, spare = [largest] + [least] * (number_of - 1), total - largest - least * (number_of - 1)
    while spare > 0:
        movable = [i for i in range(1, number_of) if counts[i] < largest] or [i for i in range(1, number_of) if counts[i] < reach]
        mass, left = sum([loads[i] for i in movable]), spare
        for i in movable:
            more = min(reach - counts[i], max(1, left * loads[i] // mass), spare)
            counts[i] = counts[i] + more
            spare = spare - more
    return np.array(counts)


def scatter_about(rng, extent, spread, reach, cuts=(), kind=jnp.bfloat16):
    array = spread * jax.random.normal(rng, extent, jnp.float32)
    if cuts:
        array = array * block_scale(rng, extent, cuts, -0.22, 0.18)
    return jnp.clip(array, -reach, reach).astype(kind)


def setup_inputs(seed: int = 0, part: int = 0) -> dict:
    keys = jax.random.split(jax.random.key(seed), 11)
    part_keys = jax.random.split(jax.random.fold_in(keys[10], part), 11)
    tokens = scatter_about(part_keys[0], (TOKENS, D), 1.0, 6.0, ((0, 32),))
    norm_gain = jnp.clip(1.0 + 0.18 * jax.random.normal(keys[1], (D,), jnp.float32), 0.1, 1.9)
    expert_gate = scatter_about(keys[2], (EXPERTS, D, FF_E), D ** -0.5, 0.125, ((0, 32), (2, 2)))
    expert_up = scatter_about(keys[3], (EXPERTS, D, FF_E), D ** -0.5, 0.125, ((0, 32), (2, 2)))
    expert_down = scatter_about(keys[4], (EXPERTS, FF_E, D), FF_E ** -0.5, 0.25, ((0, 32), (1, 2)))
    shared_gate = scatter_about(keys[5], (D, FF_S), D ** -0.5, 0.125, ((1, 2),))
    shared_up = scatter_about(keys[6], (D, FF_S), D ** -0.5, 0.125, ((1, 2),))
    shared_down = scatter_about(keys[7], (FF_S, D), FF_S ** -0.5, 0.25, ((0, 2),))
    routes_keys = jax.random.split(jax.random.fold_in(part_keys[8], 1), TOKENS // TOK_DEV)
    routes_turns = jax.random.permutation(jax.random.fold_in(part_keys[8], 3), TOKENS // TOK_DEV)
    routes = jax.vmap(lambda own, number: routed_block(jax.random.fold_in(part_keys[8], 2), own, number, TOK_DEV, EXPERTS, TOP_K, CAP, 2))(routes_keys, routes_turns).reshape((TOKENS, TOP_K))
    route_weights = jnp.clip(0.05 + 0.55 * jax.random.uniform(part_keys[9], (TOKENS, TOP_K), jnp.float32) ** block_scale(part_keys[9], (TOKENS, TOP_K), ((0, 32),), -0.2, 0.2), 0.05, 0.6)
    return dict(tokens=tokens, norm_gain=norm_gain, expert_gate=expert_gate, expert_up=expert_up, expert_down=expert_down, shared_gate=shared_gate, shared_up=shared_up, shared_down=shared_down, routes=routes, route_weights=route_weights)


def rms_scaled(values, gain):
    wide = values.astype(jnp.float32)
    scaled = wide * lax.rsqrt(lax.optimization_barrier(jnp.mean(wide * wide, axis=-1, keepdims=True)) + 1e-06)
    return (scaled * gain).astype(jnp.bfloat16)

def split_swiglu(row_block, w_gate, w_up, w_down, blocks):
    gate_proj = jnp.dot(row_block, w_gate, preferred_element_type=jnp.float32)
    up_proj = jnp.dot(row_block, w_up, preferred_element_type=jnp.float32)
    hidden = (jax.nn.silu(gate_proj) * up_proj).astype(jnp.bfloat16)
    step_width = hidden.shape[1] // blocks
    total = jnp.zeros((row_block.shape[0], w_down.shape[1]), jnp.float32)
    for block_index in range(blocks):
        lower = block_index * step_width
        partial_value = jnp.dot(hidden[:, lower:lower + step_width], w_down[lower:lower + step_width], preferred_element_type=jnp.float32)
        partial_value = lax.optimization_barrier(partial_value.astype(jnp.bfloat16))
        total = total + partial_value.astype(jnp.float32)
    return total.astype(jnp.bfloat16)

def reference(tokens, norm_gain, expert_gate, expert_up, expert_down, shared_gate, shared_up, shared_down, routes, route_weights):
    normed = rms_scaled(tokens, norm_gain)
    shared_out = split_swiglu(normed, shared_gate, shared_up, shared_down, N_TP)

    def one_expert(accum, inputs):
        w_gate, w_up, w_down, expert_index = inputs
        output = split_swiglu(normed, w_gate, w_up, w_down, N_TP)
        weight = lax.optimization_barrier(jnp.sum(jnp.where(routes == expert_index, route_weights, jnp.float32(0.0)), axis=1))
        return (accum + weight[:, None] * output.astype(jnp.float32), None)
    start = jnp.zeros(tokens.shape, jnp.float32)
    accum, unused = lax.scan(one_expert, start, (expert_gate, expert_up, expert_down, jnp.arange(EXPERTS, dtype=jnp.int32)))
    return (accum + shared_out.astype(jnp.float32)).astype(jnp.bfloat16)
```

```python
import jax
import jax.numpy as jnp
from jax import lax
from jax.sharding import PartitionSpec as P

CHAINS = 2
GROUP = 6
LANES = 128


def rms_scaled(values, gain):
    wide = values.astype(jnp.float32)
    scaled = wide * lax.rsqrt(jnp.mean(wide * wide, axis=-1, keepdims=True) + 1e-06)
    return (scaled * gain).astype(jnp.bfloat16)


def ring_pairs(ring, cores, step):
    pairs = []
    for place in range(ring):
        for core in cores:
            shift = step if core == 0 else -step
            pairs.append((place * 2 + core, (place + shift) % ring * 2 + core))
    return pairs


def passed_on(values, pairs):
    return [lax.ppermute(value, ("ep", "tp"), pairs) for value in values]


def in_turn(values, last, one):
    ready = []
    for value in values:
        if last is not None:
            value, last = lax.optimization_barrier((value, last))
        last = value * one
        ready.append(last)
    return ready, last


def weight_columns(routes, route_weights, experts):
    named = routes[:, :, None] == jnp.arange(experts, dtype=jnp.int32)[None, None, :]
    table = jnp.sum(jnp.where(named, route_weights[:, :, None], jnp.float32(0.0)), axis=1)
    head = lax.reduce_precision(table, 8, 7)
    rest = table - head
    pad = jnp.zeros((table.shape[0], LANES - 2 * experts % LANES), jnp.float32)
    return jnp.concatenate([head, rest, pad], axis=1).astype(jnp.bfloat16)


def per_device(
    tokens,
    norm_gain,
    expert_gate,
    expert_up,
    expert_down,
    shared_gate,
    shared_up,
    shared_down,
    routes,
    route_weights,
):
    rows, width = tokens.shape
    ring = lax.axis_size("ep")
    far = ring // 2
    own_expert = lax.axis_index("ep")
    core = lax.axis_index("tp")
    swap = [(0, 1), (1, 0)]
    half = width // 2

    normed = rms_scaled(tokens, norm_gain)
    columns = weight_columns(routes, route_weights, ring)
    payload = jnp.concatenate([normed, columns], axis=1)
    first = jnp.split(payload, CHAINS, axis=0)

    other_gate = lax.ppermute(expert_gate[0], "tp", swap)
    other_up = lax.ppermute(expert_up[0], "tp", swap)
    other_down = lax.ppermute(expert_down[0], "tp", swap)
    gate_up, down = lax.optimization_barrier(
        (
            jnp.concatenate([expert_gate[0], other_gate, expert_up[0], other_up], axis=1),
            jnp.concatenate([expert_down[0], other_down], axis=0),
        )
    )
    hidden_width = down.shape[0]

    lane = lax.broadcasted_iota(jnp.int32, (1, columns.shape[1]), 1)
    is_own = (lane == own_expert) | (lane == own_expert + ring)

    def expert_rows(blocks):
        merged = jnp.concatenate(blocks, axis=0)
        weight = jnp.sum(
            jnp.where(is_own, merged[:, width:].astype(jnp.float32), 0.0), axis=1, keepdims=True
        )
        proj = jnp.dot(merged[:, :width], gate_up, preferred_element_type=jnp.float32)
        hidden = (jax.nn.silu(proj[:, :hidden_width]) * proj[:, hidden_width:]).astype(jnp.bfloat16)
        out = jnp.dot(hidden, down, preferred_element_type=jnp.float32)
        return jnp.split((out * weight).astype(jnp.bfloat16), len(blocks), axis=0)

    one = (norm_gain[0] * 0.0 + 1.0).astype(jnp.bfloat16)

    both, lone = (0, 1), (1,)
    held, arrived, terms, last = first, [], [[] for _ in first], None
    for k in range(1, far + 1):
        pairs = ring_pairs(ring, both if k < far else lone, 1)
        if k > 1:
            held, last = in_turn(held, last, one)
        held = passed_on(held, pairs)
        if k == far:
            arrived.append([jnp.where(core == 1, a, b) for a, b in zip(held, first)])
        else:
            arrived.append(held)
        if k % GROUP == 0 or k == far:
            for chain in range(CHAINS):
                terms[chain] += expert_rows([blocks[chain] for blocks in arrived])
            arrived = []

    gate_proj = jnp.dot(normed, shared_gate, preferred_element_type=jnp.float32)
    up_proj = jnp.dot(normed, shared_up, preferred_element_type=jnp.float32)
    shared_hidden = (jax.nn.silu(gate_proj) * up_proj).astype(jnp.bfloat16)
    shared_part = jnp.dot(shared_hidden, shared_down, preferred_element_type=jnp.float32)

    sums = [term[-1] for term in terms]
    for k in range(far, 0, -1):
        pairs = ring_pairs(ring, lone if k == far else both, -1)
        sums = passed_on(sums, pairs)
        if k > 1:
            sums = [
                (s.astype(jnp.float32) + term[k - 2].astype(jnp.float32)).astype(jnp.bfloat16)
                for s, term in zip(sums, terms)
            ]
    own_terms = jnp.concatenate([term[-1] for term in terms], axis=0).astype(jnp.float32)
    total = jnp.concatenate(sums, axis=0).astype(jnp.float32) + shared_part
    total = total + jnp.where(core == 0, own_terms, 0.0)

    kept = jnp.where(core == 0, total[:, :half], total[:, half:])
    given = jnp.where(core == 0, total[:, half:], total[:, :half]).astype(jnp.bfloat16)
    taken = lax.ppermute(given, "tp", swap)
    return (kept + taken.astype(jnp.float32)).astype(jnp.bfloat16)


def solution(mesh):
    in_specs = (
        P(("grp", "ep"), None),
        P(),
        P("ep", None, "tp"),
        P("ep", None, "tp"),
        P("ep", "tp", None),
        P(None, "tp"),
        P(None, "tp"),
        P("tp", None),
        P(("grp", "ep"), None),
        P(("grp", "ep"), None),
    )
    out_specs = P(("grp", "ep"), "tp")
    return jax.shard_map(
        per_device, mesh=mesh, in_specs=in_specs, out_specs=out_specs, check_vma=False
    )
```

```python
import jax
import jax.numpy as jnp
from jax import lax
from jax.sharding import PartitionSpec as P

CHAINS = 1
LEAP = 8
LANES = 128


def rms_scaled(values, gain):
    wide = values.astype(jnp.float32)
    scaled = wide * lax.rsqrt(jnp.mean(wide * wide, axis=-1, keepdims=True) + 1e-06)
    return (scaled * gain).astype(jnp.bfloat16)


def ring_pairs(ring, cores, step):
    pairs = []
    for place in range(ring):
        for core in cores:
            shift = step if core == 0 else -step
            pairs.append((place * 2 + core, (place + shift) % ring * 2 + core))
    return pairs


def moved(value, ring, cores, step):
    return lax.ppermute(value, ("ep", "tp"), ring_pairs(ring, cores, step))


def weight_columns(routes, route_weights, experts):
    named = routes[:, :, None] == jnp.arange(experts, dtype=jnp.int32)[None, None, :]
    table = jnp.sum(jnp.where(named, route_weights[:, :, None], jnp.float32(0.0)), axis=1)
    head = lax.reduce_precision(table, 8, 7)
    rest = table - head
    pad = jnp.zeros((table.shape[0], LANES - 2 * experts % LANES), jnp.float32)
    return jnp.concatenate([head, rest, pad], axis=1).astype(jnp.bfloat16)


def per_device(
    tokens,
    norm_gain,
    expert_gate,
    expert_up,
    expert_down,
    shared_gate,
    shared_up,
    shared_down,
    routes,
    route_weights,
):
    _, width = tokens.shape
    ring = lax.axis_size("ep")
    far = ring // 2
    own_expert = lax.axis_index("ep")
    core = lax.axis_index("tp")
    swap = [(0, 1), (1, 0)]
    half = width // 2

    normed = rms_scaled(tokens, norm_gain)
    columns = weight_columns(routes, route_weights, ring)
    payload = jnp.concatenate([normed, columns], axis=1)
    first = jnp.split(payload, CHAINS, axis=0)

    gate_proj = jnp.dot(normed, shared_gate, preferred_element_type=jnp.float32)
    up_proj = jnp.dot(normed, shared_up, preferred_element_type=jnp.float32)
    shared_hidden = (jax.nn.silu(gate_proj) * up_proj).astype(jnp.bfloat16)
    shared_part = jnp.dot(shared_hidden, shared_down, preferred_element_type=jnp.float32)

    other_gate = lax.ppermute(expert_gate[0], "tp", swap)
    other_up = lax.ppermute(expert_up[0], "tp", swap)
    other_down = lax.ppermute(expert_down[0], "tp", swap)
    gate_up, down = lax.optimization_barrier(
        (
            jnp.concatenate([expert_gate[0], other_gate, expert_up[0], other_up], axis=1),
            jnp.concatenate([expert_down[0], other_down], axis=0),
        )
    )
    hidden_width = down.shape[0]

    lane = lax.broadcasted_iota(jnp.int32, (1, columns.shape[1]), 1)
    is_own = (lane == own_expert) | (lane == own_expert + ring)

    def expert_rows(blocks):
        merged = jnp.concatenate(blocks, axis=0)
        weight = jnp.sum(
            jnp.where(is_own, merged[:, width:].astype(jnp.float32), 0.0), axis=1, keepdims=True
        )
        proj = jnp.dot(merged[:, :width], gate_up, preferred_element_type=jnp.float32)
        hidden = (jax.nn.silu(proj[:, :hidden_width]) * proj[:, hidden_width:]).astype(jnp.bfloat16)
        out = jnp.dot(hidden, down, preferred_element_type=jnp.float32)
        return jnp.split((out * weight).astype(jnp.bfloat16), len(blocks), axis=0)

    one = (core < 2).astype(jnp.bfloat16)
    both, lone = (0, 1), (1,)
    last = [one]

    def in_turn(step, *values):
        *tied, _ = lax.optimization_barrier((*values, last[0]))
        last[0] = step(*tied)
        return (last[0], *tied)

    blocks = [[None] * (far + 1) for _ in first]
    for chain, block in enumerate(first):
        blocks[chain][LEAP] = moved(block, ring, both, LEAP)
        blocks[chain][1] = moved(block, ring, both, 1)
    order = []
    near, distant = list(range(2, LEAP)), list(range(LEAP + 1, far + 1))
    while near or distant:
        order += distant[:1] + near[:1]
        near, distant = near[1:], distant[1:]
    for k in order:
        for chain in range(CHAINS):
            block, arrived = in_turn(lambda b: b * one, blocks[chain][k - 1])
            if k == LEAP + 1:
                blocks[chain][LEAP] = arrived
            blocks[chain][k] = moved(block, ring, both if k < far else lone, 1)
    for chain, block in enumerate(first):
        blocks[chain][far] = jnp.where(core == 1, blocks[chain][far], block)

    terms = [[None] * (far + 1) for _ in first]
    middle, turn = LEAP // 2 + 1, (LEAP + far) // 2 + 1
    early = [*range(1, middle), *range(LEAP, turn)]
    late = [*range(middle, LEAP), *range(turn, far + 1)]
    for group in (early, late):
        for chain in range(CHAINS):
            made = expert_rows([blocks[chain][k] for k in group])
            for k, term in zip(group, made):
                terms[chain][k] = term

    def added(s, t):
        return (s.astype(jnp.float32) + t.astype(jnp.float32)).astype(jnp.bfloat16)

    distant = [moved(term[far], ring, lone, -1) for term in terms]
    near = [moved(term[LEAP - 1], ring, both, -1) for term in terms]
    for i in range(1, max(far - LEAP, LEAP - 2) + 1):
        for chain, term in enumerate(terms):
            if i <= far - LEAP:
                total, *_ = in_turn(added, distant[chain], term[far - i])
                leap = LEAP if i == far - LEAP else 1
                distant[chain] = moved(total, ring, both, -leap)
            if i <= LEAP - 2:
                total, *_ = in_turn(added, near[chain], term[LEAP - 1 - i])
                near[chain] = moved(total, ring, both, -1)
    own_terms = jnp.concatenate([term[far] for term in terms], axis=0).astype(jnp.float32)
    total = jnp.concatenate(near, axis=0).astype(jnp.float32) + shared_part
    total = total + jnp.where(core == 0, own_terms, 0.0)
    total = total + jnp.concatenate(distant, axis=0).astype(jnp.float32)

    kept = jnp.where(core == 0, total[:, :half], total[:, half:])
    given = jnp.where(core == 0, total[:, half:], total[:, :half]).astype(jnp.bfloat16)
    taken = lax.ppermute(given, "tp", swap)
    return (kept + taken.astype(jnp.float32)).astype(jnp.bfloat16)


def solution(mesh):
    in_specs = (
        P(("grp", "ep"), None),
        P(),
        P("ep", None, "tp"),
        P("ep", None, "tp"),
        P("ep", "tp", None),
        P(None, "tp"),
        P(None, "tp"),
        P("tp", None),
        P(("grp", "ep"), None),
        P(("grp", "ep"), None),
    )
    out_specs = P(("grp", "ep"), "tp")

    return jax.shard_map(per_device, mesh=mesh, in_specs=in_specs, out_specs=out_specs, check_vma=False)
```

```python
import jax
import jax.numpy as jnp
from jax import lax
from jax.sharding import PartitionSpec as P

CHAINS = 1
LEAP = 8
LANES = 128


def rms_scaled(values, gain):
    wide = values.astype(jnp.float32)
    scaled = wide * lax.rsqrt(jnp.mean(wide * wide, axis=-1, keepdims=True) + 1e-06)
    return (scaled * gain).astype(jnp.bfloat16)


def ring_pairs(ring, cores, step, crossed=False):
    pairs = []
    for place in range(ring):
        for core in cores:
            shift = step if core == 0 else -step
            target = 1 - core if crossed else core
            pairs.append((place * 2 + core, (place + shift) % ring * 2 + target))
    return pairs


def moved(value, ring, cores, step, crossed=False):
    return lax.ppermute(value, ("ep", "tp"), ring_pairs(ring, cores, step, crossed))


def weight_columns(routes, route_weights, experts):
    named = routes[:, :, None] == jnp.arange(experts, dtype=jnp.int32)[None, None, :]
    table = jnp.sum(jnp.where(named, route_weights[:, :, None], jnp.float32(0.0)), axis=1)
    head = lax.reduce_precision(table, 8, 7)
    rest = table - head
    pad = jnp.zeros((table.shape[0], LANES - 2 * experts % LANES), jnp.float32)
    return jnp.concatenate([head, rest, pad], axis=1).astype(jnp.bfloat16)


def per_device(
    tokens,
    norm_gain,
    expert_gate,
    expert_up,
    expert_down,
    shared_gate,
    shared_up,
    shared_down,
    routes,
    route_weights,
):
    _, width = tokens.shape
    ring = lax.axis_size("ep")
    far = ring // 2
    own_expert = lax.axis_index("ep")
    core = lax.axis_index("tp")
    swap = [(0, 1), (1, 0)]
    half = width // 2

    normed = rms_scaled(tokens, norm_gain)
    columns = weight_columns(routes, route_weights, ring)
    payload = jnp.concatenate([normed, columns], axis=1)
    first = jnp.split(payload, CHAINS, axis=0)

    gate_proj = jnp.dot(normed, shared_gate, preferred_element_type=jnp.float32)
    up_proj = jnp.dot(normed, shared_up, preferred_element_type=jnp.float32)
    shared_hidden = (jax.nn.silu(gate_proj) * up_proj).astype(jnp.bfloat16)
    shared_part = jnp.dot(shared_hidden, shared_down, preferred_element_type=jnp.float32)
    shared_part = lax.optimization_barrier(shared_part)

    other_gate = lax.ppermute(expert_gate[0], "tp", swap)
    other_up = lax.ppermute(expert_up[0], "tp", swap)
    other_down = lax.ppermute(expert_down[0], "tp", swap)
    gate_up = jnp.concatenate([expert_gate[0], other_gate, expert_up[0], other_up], axis=1)
    down = jnp.concatenate([expert_down[0], other_down], axis=0)
    gate_up, down = lax.optimization_barrier((gate_up, down))
    hidden_width = down.shape[0]

    lane = lax.broadcasted_iota(jnp.int32, (1, columns.shape[1]), 1)
    is_own = (lane == own_expert) | (lane == own_expert + ring)

    def expert_rows(blocks):
        merged = jnp.concatenate(blocks, axis=0)
        weight = jnp.sum(
            jnp.where(is_own, merged[:, width:].astype(jnp.float32), 0.0), axis=1, keepdims=True
        )
        proj = jnp.dot(merged[:, :width], gate_up, preferred_element_type=jnp.float32)
        hidden = (jax.nn.silu(proj[:, :hidden_width]) * proj[:, hidden_width:]).astype(jnp.bfloat16)
        out = jnp.dot(hidden, down, preferred_element_type=jnp.float32)
        return jnp.split((out * weight).astype(jnp.bfloat16), len(blocks), axis=0)

    one = (core < 2).astype(jnp.bfloat16)
    both, lone = (0, 1), (1,)
    last = [one]

    def in_turn(step, *values):
        *tied, _ = lax.optimization_barrier((*values, last[0]))
        last[0] = step(*tied)
        return (last[0], *tied)

    blocks = [[None] * (far + 1) for _ in first]
    for chain, block in enumerate(first):
        blocks[chain][LEAP] = moved(block, ring, both, LEAP)
        blocks[chain][1] = moved(block, ring, both, 1)
    order = []
    near, distant = list(range(2, LEAP)), list(range(LEAP + 1, far + 1))
    while near or distant:
        order += distant[:1] + near[:1]
        near, distant = near[1:], distant[1:]
    for k in order:
        for chain in range(CHAINS):
            block, arrived = in_turn(lambda b: b * one, blocks[chain][k - 1])
            if k == LEAP + 1:
                blocks[chain][LEAP] = arrived
            blocks[chain][k] = moved(block, ring, both if k < far else lone, 1)
    for chain, block in enumerate(first):
        blocks[chain][far] = jnp.where(core == 1, blocks[chain][far], block)

    terms = [[None] * (far + 1) for _ in first]
    middle, turn = LEAP // 2 + 1, (LEAP + far) // 2 + 1
    early = [*range(1, middle), *range(LEAP, turn)]
    late = [*range(middle, LEAP), *range(turn, far + 1)]
    for group in (early, late):
        for chain in range(CHAINS):
            made = expert_rows([blocks[chain][k] for k in group])
            for k, term in zip(group, made):
                terms[chain][k] = term

    def halves(value):
        left, right = value[:, :half], value[:, half:]
        return jnp.where(core == 0, left, right), jnp.where(core == 0, right, left)

    def added(s, t):
        return (s.astype(jnp.float32) + t.astype(jnp.float32)).astype(jnp.bfloat16)

    distant = [moved(term[far], ring, lone, -1) for term in terms]
    near = [moved(term[LEAP - 1], ring, both, -1) for term in terms]
    for i in range(1, max(far - LEAP, LEAP - 2) + 1):
        for chain, term in enumerate(terms):
            if i <= far - LEAP:
                total, *_ = in_turn(added, distant[chain], term[far - i])
                if i < far - LEAP:
                    distant[chain] = moved(total, ring, both, -1)
                else:
                    straight, crossed = halves(total)
                    straight = moved(straight, ring, both, -LEAP)
                    crossed = moved(crossed, ring, both, -LEAP, crossed=True)
                    distant[chain] = straight.astype(jnp.float32) + crossed.astype(jnp.float32)
            if i <= LEAP - 2:
                total, *_ = in_turn(added, near[chain], term[LEAP - 1 - i])
                near[chain] = moved(total, ring, both, -1)
    own_terms = jnp.concatenate([term[far] for term in terms], axis=0).astype(jnp.float32)
    total = jnp.concatenate(near, axis=0).astype(jnp.float32) + shared_part
    kept, given = halves(total + jnp.where(core == 0, own_terms, 0.0))
    kept, given = lax.optimization_barrier((kept, given.astype(jnp.bfloat16)))
    taken = lax.ppermute(given, "tp", swap)
    kept = lax.optimization_barrier(kept + taken.astype(jnp.float32))
    return (kept + jnp.concatenate(distant, axis=0)).astype(jnp.bfloat16)


def solution(mesh):
    in_specs = (
        P(("grp", "ep"), None),
        P(),
        P("ep", None, "tp"),
        P("ep", None, "tp"),
        P("ep", "tp", None),
        P(None, "tp"),
        P(None, "tp"),
        P("tp", None),
        P(("grp", "ep"), None),
        P(("grp", "ep"), None),
    )
    out_specs = P(("grp", "ep"), "tp")

    return jax.shard_map(per_device, mesh=mesh, in_specs=in_specs, out_specs=out_specs, check_vma=False)
```

```python
import jax
import jax.numpy as jnp
from jax import lax
from jax.sharding import PartitionSpec as P

CHAINS = 2
LEAP = 8
LANES = 128


def rms_scaled(values, gain):
    wide = values.astype(jnp.float32)
    scaled = wide * lax.rsqrt(jnp.mean(wide * wide, axis=-1, keepdims=True) + 1e-06)
    return (scaled * gain).astype(jnp.bfloat16)


def ring_pairs(ring, cores, step):
    pairs = []
    for place in range(ring):
        for core in cores:
            shift = step if core == 0 else -step
            pairs.append((place * 2 + core, (place + shift) % ring * 2 + core))
    return pairs


def moved(value, ring, cores, step):
    return lax.ppermute(value, ("ep", "tp"), ring_pairs(ring, cores, step))


def weight_columns(routes, route_weights, experts):
    named = routes[:, :, None] == jnp.arange(experts, dtype=jnp.int32)[None, None, :]
    table = jnp.sum(jnp.where(named, route_weights[:, :, None], jnp.float32(0.0)), axis=1)
    head = lax.reduce_precision(table, 8, 7)
    rest = table - head
    pad = jnp.zeros((table.shape[0], LANES - 2 * experts % LANES), jnp.float32)
    return jnp.concatenate([head, rest, pad], axis=1).astype(jnp.bfloat16)


def per_device(
    tokens,
    norm_gain,
    expert_gate,
    expert_up,
    expert_down,
    shared_gate,
    shared_up,
    shared_down,
    routes,
    route_weights,
):
    _, width = tokens.shape
    ring = lax.axis_size("ep")
    far = ring // 2
    own_expert = lax.axis_index("ep")
    core = lax.axis_index("tp")
    swap = [(0, 1), (1, 0)]
    half = width // 2

    normed = rms_scaled(tokens, norm_gain)
    columns = weight_columns(routes, route_weights, ring)
    payload = jnp.concatenate([normed, columns], axis=1)
    first = jnp.split(payload, CHAINS, axis=0)

    gate_proj = jnp.dot(normed, shared_gate, preferred_element_type=jnp.float32)
    up_proj = jnp.dot(normed, shared_up, preferred_element_type=jnp.float32)
    shared_hidden = (jax.nn.silu(gate_proj) * up_proj).astype(jnp.bfloat16)
    shared_part = jnp.dot(shared_hidden, shared_down, preferred_element_type=jnp.float32)
    shared_part = lax.optimization_barrier(shared_part)

    other_gate = lax.ppermute(expert_gate[0], "tp", swap)
    other_up = lax.ppermute(expert_up[0], "tp", swap)
    other_down = lax.ppermute(expert_down[0], "tp", swap)
    gate_up = jnp.concatenate([expert_gate[0], other_gate, expert_up[0], other_up], axis=1)
    down = jnp.concatenate([expert_down[0], other_down], axis=0)
    gate_up, down = lax.optimization_barrier((gate_up, down))
    hidden_width = down.shape[0]

    lane = lax.broadcasted_iota(jnp.int32, (1, columns.shape[1]), 1)
    is_own = (lane == own_expert) | (lane == own_expert + ring)

    def expert_rows(blocks):
        merged = jnp.concatenate(blocks, axis=0)
        weight = jnp.sum(
            jnp.where(is_own, merged[:, width:].astype(jnp.float32), 0.0), axis=1, keepdims=True
        )
        proj = jnp.dot(merged[:, :width], gate_up, preferred_element_type=jnp.float32)
        hidden = (jax.nn.silu(proj[:, :hidden_width]) * proj[:, hidden_width:]).astype(jnp.bfloat16)
        out = jnp.dot(hidden, down, preferred_element_type=jnp.float32)
        return jnp.split((out * weight).astype(jnp.bfloat16), len(blocks), axis=0)

    one = (core < 2).astype(jnp.bfloat16)
    both, lone = (0, 1), (1,)
    last = [one]

    def in_turn(step, *values):
        *tied, _ = lax.optimization_barrier((*values, last[0]))
        last[0] = step(*tied)
        return (last[0], *tied)

    blocks = [[None] * (far + 1) for _ in first]
    for chain, block in enumerate(first):
        blocks[chain][LEAP] = moved(block, ring, both, LEAP)
        blocks[chain][1] = moved(block, ring, both, 1)
    order = []
    near, distant = list(range(2, LEAP)), list(range(LEAP + 1, far + 1))
    while near or distant:
        order += distant[:1] + near[:1]
        near, distant = near[1:], distant[1:]
    for k in order:
        for chain in range(CHAINS):
            block, arrived = in_turn(lambda b: b * one, blocks[chain][k - 1])
            if k == LEAP + 1:
                blocks[chain][LEAP] = arrived
            blocks[chain][k] = moved(block, ring, both if k < far else lone, 1)
    for chain, block in enumerate(first):
        blocks[chain][far] = jnp.where(core == 1, blocks[chain][far], block)

    terms = [[None] * (far + 1) for _ in first]
    middle, turn = LEAP // 2 + 1, (LEAP + far) // 2 + 1
    early = [*range(1, middle), *range(LEAP, turn)]
    late = [*range(middle, LEAP), *range(turn, far + 1)]
    for group in (early, late):
        for chain in range(CHAINS):
            made = expert_rows([blocks[chain][k] for k in group])
            for k, term in zip(group, made):
                terms[chain][k] = term

    def added(s, t):
        return (s.astype(jnp.float32) + t.astype(jnp.float32)).astype(jnp.bfloat16)

    distant = [moved(term[far], ring, lone, -1) for term in terms]
    near = [moved(term[LEAP - 1], ring, both, -1) for term in terms]
    for i in range(1, max(far - LEAP, LEAP - 2) + 1):
        for chain, term in enumerate(terms):
            if i <= far - LEAP:
                total, *_ = in_turn(added, distant[chain], term[far - i])
                leap = LEAP if i == far - LEAP else 1
                distant[chain] = moved(total, ring, both, -leap)
            if i <= LEAP - 2:
                total, *_ = in_turn(added, near[chain], term[LEAP - 1 - i])
                near[chain] = moved(total, ring, both, -1)
    own_terms = jnp.concatenate([term[far] for term in terms], axis=0).astype(jnp.float32)
    total = jnp.concatenate(near, axis=0).astype(jnp.float32) + shared_part
    total = lax.optimization_barrier(total + jnp.where(core == 0, own_terms, 0.0))
    total = total + jnp.concatenate(distant, axis=0).astype(jnp.float32)
    kept = jnp.where(core == 0, total[:, :half], total[:, half:])
    given = jnp.where(core == 0, total[:, half:], total[:, :half]).astype(jnp.bfloat16)
    taken = lax.ppermute(given, "tp", swap)
    return (kept + taken.astype(jnp.float32)).astype(jnp.bfloat16)


def solution(mesh):
    in_specs = (
        P(("grp", "ep"), None),
        P(),
        P("ep", None, "tp"),
        P("ep", None, "tp"),
        P("ep", "tp", None),
        P(None, "tp"),
        P(None, "tp"),
        P("tp", None),
        P(("grp", "ep"), None),
        P(("grp", "ep"), None),
    )
    out_specs = P(("grp", "ep"), "tp")

    return jax.shard_map(per_device, mesh=mesh, in_specs=in_specs, out_specs=out_specs, check_vma=False)
```

```python
import jax
import jax.numpy as jnp
from jax import lax
from jax.sharding import PartitionSpec as P

CHAINS = 1
LEAP = 8
LATE = 2
LANES = 128


def rms_scaled(values, gain):
    wide = values.astype(jnp.float32)
    scaled = wide * lax.rsqrt(jnp.mean(wide * wide, axis=-1, keepdims=True) + 1e-06)
    return (scaled * gain).astype(jnp.bfloat16)


def ring_pairs(ring, cores, step):
    pairs = []
    for place in range(ring):
        for core in cores:
            shift = step if core == 0 else -step
            pairs.append((place * 2 + core, (place + shift) % ring * 2 + core))
    return pairs


def moved(value, ring, cores, step):
    return lax.ppermute(value, ("ep", "tp"), ring_pairs(ring, cores, step))


def weight_columns(routes, route_weights, experts):
    named = routes[:, :, None] == jnp.arange(experts, dtype=jnp.int32)[None, None, :]
    table = jnp.sum(jnp.where(named, route_weights[:, :, None], jnp.float32(0.0)), axis=1)
    head = lax.reduce_precision(table, 8, 7)
    rest = table - head
    pad = jnp.zeros((table.shape[0], LANES - 2 * experts % LANES), jnp.float32)
    return jnp.concatenate([head, rest, pad], axis=1).astype(jnp.bfloat16)


def per_device(
    tokens,
    norm_gain,
    expert_gate,
    expert_up,
    expert_down,
    shared_gate,
    shared_up,
    shared_down,
    routes,
    route_weights,
):
    _, width = tokens.shape
    ring = lax.axis_size("ep")
    far = ring // 2
    own_expert = lax.axis_index("ep")
    core = lax.axis_index("tp")
    swap = [(0, 1), (1, 0)]
    half = width // 2

    normed = rms_scaled(tokens, norm_gain)
    columns = weight_columns(routes, route_weights, ring)
    payload = jnp.concatenate([normed, columns], axis=1)
    first = jnp.split(payload, CHAINS, axis=0)

    gate_proj = jnp.dot(normed, shared_gate, preferred_element_type=jnp.float32)
    up_proj = jnp.dot(normed, shared_up, preferred_element_type=jnp.float32)
    shared_hidden = (jax.nn.silu(gate_proj) * up_proj).astype(jnp.bfloat16)
    shared_part = jnp.dot(shared_hidden, shared_down, preferred_element_type=jnp.float32)
    shared_part = lax.optimization_barrier(shared_part)

    other_gate = lax.ppermute(expert_gate[0], "tp", swap)
    other_up = lax.ppermute(expert_up[0], "tp", swap)
    other_down = lax.ppermute(expert_down[0], "tp", swap)
    gate_up = jnp.concatenate([expert_gate[0], other_gate, expert_up[0], other_up], axis=1)
    down = jnp.concatenate([expert_down[0], other_down], axis=0)
    gate_up, down = lax.optimization_barrier((gate_up, down))
    hidden_width = down.shape[0]

    lane = lax.broadcasted_iota(jnp.int32, (1, columns.shape[1]), 1)
    is_own = (lane == own_expert) | (lane == own_expert + ring)

    def expert_rows(blocks):
        merged = jnp.concatenate(blocks, axis=0)
        weight = jnp.sum(
            jnp.where(is_own, merged[:, width:].astype(jnp.float32), 0.0), axis=1, keepdims=True
        )
        proj = jnp.dot(merged[:, :width], gate_up, preferred_element_type=jnp.float32)
        hidden = (jax.nn.silu(proj[:, :hidden_width]) * proj[:, hidden_width:]).astype(jnp.bfloat16)
        out = jnp.dot(hidden, down, preferred_element_type=jnp.float32)
        return jnp.split((out * weight).astype(jnp.bfloat16), len(blocks), axis=0)

    one = (core < 2).astype(jnp.bfloat16)
    both, lone = (0, 1), (1,)
    last = [one]

    def in_turn(step, *values):
        *tied, _ = lax.optimization_barrier((*values, last[0]))
        last[0] = step(*tied)
        return (last[0], *tied)

    blocks = [[None] * (far + 1) for _ in first]
    for chain, block in enumerate(first):
        blocks[chain][LEAP] = moved(block, ring, both, LEAP)
        blocks[chain][1] = moved(block, ring, both, 1)
    order = []
    near, distant = list(range(2, LEAP)), list(range(LEAP + 1, far + 1))
    while near or distant:
        order += distant[:1] + near[:1]
        near, distant = near[1:], distant[1:]
    for k in order:
        for chain in range(CHAINS):
            block, arrived = in_turn(lambda b: b * one, blocks[chain][k - 1])
            if k == LEAP + 1:
                blocks[chain][LEAP] = arrived
            blocks[chain][k] = moved(block, ring, both if k < far else lone, 1)
    for chain, block in enumerate(first):
        blocks[chain][far] = jnp.where(core == 1, blocks[chain][far], block)

    terms = [[None] * (far + 1) for _ in first]
    middle, turn = LEAP - LATE, far + 1 - LATE - 1
    early = [*range(1, middle), *range(LEAP, turn)]
    late = [*range(middle, LEAP), *range(turn, far + 1)]
    for group in (early, late):
        for chain in range(CHAINS):
            made = expert_rows([blocks[chain][k] for k in group])
            for k, term in zip(group, made):
                terms[chain][k] = term

    def added(s, t):
        return (s.astype(jnp.float32) + t.astype(jnp.float32)).astype(jnp.bfloat16)

    distant = [moved(term[far], ring, lone, -1) for term in terms]
    near = [moved(term[LEAP - 1], ring, both, -1) for term in terms]
    for i in range(1, max(far - LEAP, LEAP - 2) + 1):
        for chain, term in enumerate(terms):
            if i <= far - LEAP:
                total, *_ = in_turn(added, distant[chain], term[far - i])
                leap = LEAP if i == far - LEAP else 1
                distant[chain] = moved(total, ring, both, -leap)
            if i <= LEAP - 2:
                total, *_ = in_turn(added, near[chain], term[LEAP - 1 - i])
                near[chain] = moved(total, ring, both, -1)

    def halves(value):
        left, right = value[:, :half], value[:, half:]
        return jnp.where(core == 0, left, right), jnp.where(core == 0, right, left)

    own_terms = jnp.concatenate([term[far] for term in terms], axis=0).astype(jnp.float32)
    total = jnp.concatenate(near, axis=0).astype(jnp.float32) + shared_part
    kept, given = halves(total + jnp.where(core == 0, own_terms, 0.0))
    kept, given = lax.optimization_barrier((kept, given))
    mine, theirs = halves(jnp.concatenate(distant, axis=0))
    taken = lax.ppermute((given + theirs.astype(jnp.float32)).astype(jnp.bfloat16), "tp", swap)
    return (kept + mine.astype(jnp.float32) + taken.astype(jnp.float32)).astype(jnp.bfloat16)


def solution(mesh):
    in_specs = (
        P(("grp", "ep"), None),
        P(),
        P("ep", None, "tp"),
        P("ep", None, "tp"),
        P("ep", "tp", None),
        P(None, "tp"),
        P(None, "tp"),
        P("tp", None),
        P(("grp", "ep"), None),
        P(("grp", "ep"), None),
    )
    out_specs = P(("grp", "ep"), "tp")

    return jax.shard_map(per_device, mesh=mesh, in_specs=in_specs, out_specs=out_specs, check_vma=False)
```

```python
import jax
import jax.numpy as jnp
from jax import lax
from jax.sharding import PartitionSpec as P

CHAINS = 1
LEAP = 8
LATE = 2
LANES = 128


def rms_scaled(values, gain):
    wide = values.astype(jnp.float32)
    scaled = wide * lax.rsqrt(jnp.mean(wide * wide, axis=-1, keepdims=True) + 1e-06)
    return (scaled * gain).astype(jnp.bfloat16)


def ring_pairs(ring, flows, places, change, back):
    before, after = change
    pairs = []
    for place in range(ring):
        for flow in flows:
            shift = places if flow == 0 else -places
            source = place * 2 + (before ^ flow)
            target = (place + shift) % ring * 2 + (after ^ flow)
            pairs.append((target, source) if back else (source, target))
    return pairs


def moved(value, ring, flows, k, back=False):
    if k == LEAP:
        pairs = ring_pairs(ring, flows, LEAP, (0, 0), back)
    else:
        on = (k if k < LEAP else k - LEAP) % 2
        pairs = ring_pairs(ring, flows, 1, (1 - on, on), back)
    return lax.ppermute(value, ("ep", "tp"), pairs)


def weight_columns(routes, route_weights, experts):
    named = routes[:, :, None] == jnp.arange(experts, dtype=jnp.int32)[None, None, :]
    table = jnp.sum(jnp.where(named, route_weights[:, :, None], jnp.float32(0.0)), axis=1)
    head = lax.reduce_precision(table, 8, 7)
    rest = table - head
    pad = jnp.zeros((table.shape[0], LANES - 2 * experts % LANES), jnp.float32)
    return jnp.concatenate([head, rest, pad], axis=1).astype(jnp.bfloat16)


def per_device(
    tokens,
    norm_gain,
    expert_gate,
    expert_up,
    expert_down,
    shared_gate,
    shared_up,
    shared_down,
    routes,
    route_weights,
):
    _, width = tokens.shape
    ring = lax.axis_size("ep")
    far = ring // 2
    own_expert = lax.axis_index("ep")
    core = lax.axis_index("tp")
    swap = [(0, 1), (1, 0)]
    half = width // 2

    normed = rms_scaled(tokens, norm_gain)
    columns = weight_columns(routes, route_weights, ring)
    payload = jnp.concatenate([normed, columns], axis=1)
    first = jnp.split(payload, CHAINS, axis=0)

    gate_proj = jnp.dot(normed, shared_gate, preferred_element_type=jnp.float32)
    up_proj = jnp.dot(normed, shared_up, preferred_element_type=jnp.float32)
    shared_hidden = (jax.nn.silu(gate_proj) * up_proj).astype(jnp.bfloat16)
    shared_part = jnp.dot(shared_hidden, shared_down, preferred_element_type=jnp.float32)
    shared_part = lax.optimization_barrier(shared_part)

    other_gate = lax.ppermute(expert_gate[0], "tp", swap)
    other_up = lax.ppermute(expert_up[0], "tp", swap)
    other_down = lax.ppermute(expert_down[0], "tp", swap)
    gate_up = jnp.concatenate([expert_gate[0], other_gate, expert_up[0], other_up], axis=1)
    down = jnp.concatenate([expert_down[0], other_down], axis=0)
    gate_up, down = lax.optimization_barrier((gate_up, down))
    hidden_width = down.shape[0]

    lane = lax.broadcasted_iota(jnp.int32, (1, columns.shape[1]), 1)
    is_own = (lane == own_expert) | (lane == own_expert + ring)

    def expert_rows(blocks):
        merged = jnp.concatenate(blocks, axis=0)
        weight = jnp.sum(
            jnp.where(is_own, merged[:, width:].astype(jnp.float32), 0.0), axis=1, keepdims=True
        )
        proj = jnp.dot(merged[:, :width], gate_up, preferred_element_type=jnp.float32)
        hidden = (jax.nn.silu(proj[:, :hidden_width]) * proj[:, hidden_width:]).astype(jnp.bfloat16)
        out = jnp.dot(hidden, down, preferred_element_type=jnp.float32)
        return jnp.split((out * weight).astype(jnp.bfloat16), len(blocks), axis=0)

    one = (core < 2).astype(jnp.bfloat16)
    both, lone = (0, 1), (1,)
    last = [one]

    def in_turn(step, *values):
        *tied, _ = lax.optimization_barrier((*values, last[0]))
        last[0] = step(*tied)
        return (last[0], *tied)

    blocks = [[None] * (far + 1) for _ in first]
    for chain, block in enumerate(first):
        blocks[chain][LEAP] = moved(block, ring, both, LEAP)
        blocks[chain][1] = moved(block, ring, both, 1)
    order = []
    near, distant = list(range(2, LEAP)), list(range(LEAP + 1, far + 1))
    while near or distant:
        order += distant[:1] + near[:1]
        near, distant = near[1:], distant[1:]
    for k in order:
        for chain in range(CHAINS):
            block, arrived = in_turn(lambda b: b * one, blocks[chain][k - 1])
            if k == LEAP + 1:
                blocks[chain][LEAP] = arrived
            blocks[chain][k] = moved(block, ring, both if k < far else lone, k)
    for chain, block in enumerate(first):
        blocks[chain][far] = jnp.where(core == 1, blocks[chain][far], block)

    terms = [[None] * (far + 1) for _ in first]
    middle, turn = LEAP - LATE, far + 1 - LATE - 1
    early = [*range(1, middle), *range(LEAP, turn)]
    late = [*range(middle, LEAP), *range(turn, far + 1)]
    for group in (early, late):
        for chain in range(CHAINS):
            made = expert_rows([blocks[chain][k] for k in group])
            for k, term in zip(group, made):
                terms[chain][k] = term

    def added(s, t):
        return (s.astype(jnp.float32) + t.astype(jnp.float32)).astype(jnp.bfloat16)

    distant = [moved(term[far], ring, lone, far, back=True) for term in terms]
    near = [moved(term[LEAP - 1], ring, both, LEAP - 1, back=True) for term in terms]
    for i in range(1, max(far - LEAP, LEAP - 2) + 1):
        for chain, term in enumerate(terms):
            if i <= far - LEAP:
                total, *_ = in_turn(added, distant[chain], term[far - i])
                distant[chain] = moved(total, ring, both, far - i, back=True)
            if i <= LEAP - 2:
                total, *_ = in_turn(added, near[chain], term[LEAP - 1 - i])
                near[chain] = moved(total, ring, both, LEAP - 1 - i, back=True)

    def halves(value):
        left, right = value[:, :half], value[:, half:]
        return jnp.where(core == 0, left, right), jnp.where(core == 0, right, left)

    own_terms = jnp.concatenate([term[far] for term in terms], axis=0).astype(jnp.float32)
    total = jnp.concatenate(near, axis=0).astype(jnp.float32) + shared_part
    kept, given = halves(total + jnp.where(core == 0, own_terms, 0.0))
    kept, given = lax.optimization_barrier((kept, given))
    mine, theirs = halves(jnp.concatenate(distant, axis=0))
    taken = lax.ppermute((given + theirs.astype(jnp.float32)).astype(jnp.bfloat16), "tp", swap)
    return (kept + mine.astype(jnp.float32) + taken.astype(jnp.float32)).astype(jnp.bfloat16)


def solution(mesh):
    in_specs = (
        P(("grp", "ep"), None),
        P(),
        P("ep", None, "tp"),
        P("ep", None, "tp"),
        P("ep", "tp", None),
        P(None, "tp"),
        P(None, "tp"),
        P("tp", None),
        P(("grp", "ep"), None),
        P(("grp", "ep"), None),
    )
    out_specs = P(("grp", "ep"), "tp")

    return jax.shard_map(per_device, mesh=mesh, in_specs=in_specs, out_specs=out_specs, check_vma=False)
```
